32 devices in a mesh: rep: 2 (over x), fs: 8 (over z, y), tp: 2 (over core).
Axes of the slice: x: 2, y: 2, z: 4, core: 2. Of those that a mesh axis runs over, the one named last changes fastest.
Arguments:
- residual: bfloat16 [8192, 2048], P(('rep', 'fs', 'tp')), may hold values from -6 to 6
- mixer_gain: float32 [2048], replicated, may hold values from 0.1 to 1.9
- gating_proj: bfloat16 [2048, 2048], P('fs', 'tp'), may hold values from -0.125 to 0.125
- spatial_proj: bfloat16 [2048, 2048], P('fs', 'tp'), as said below
- spatial_gain: float32 [2048], replicated, may hold values from 0.1 to 1.9
- spatial_bias: float32 [2048], replicated, may hold values from -3 to 3
- spatial_mix: bfloat16 [32, 128, 128], replicated, may hold values from -0.5 to 0.5
- spatial_offset: float32 [32, 128], replicated, may hold values from 0.5 to 1.5
- mixer_out: bfloat16 [2048, 2048], P('tp', 'fs'), may hold values from -0.125 to 0.125
- channel_gain: float32 [2048], replicated, may hold values from 0.1 to 1.9
- gate_proj: bfloat16 [2048, 2816], P('fs', 'tp'), may hold values from -0.125 to 0.125
- up_proj: bfloat16 [2048, 2816], P('fs', 'tp'), may hold values from -0.125 to 0.125
- conv_taps: float32 [3, 2816], replicated, may hold values from -3.5 to 3.5
- down_proj: bfloat16 [2816, 2048], P('tp', 'fs'), may hold values from -0.109375 to 0.109375
Outputs:
- layer_out: bfloat16 [8192, 2048], P(('rep', 'fs', 'tp'))
The draws below stay inside these ranges and needn't reach their ends.
Inputs may be any that keep to these rules, and one draw needn't show every extreme that they name: `spatial_proj`: entries are bounded in magnitude by 56 / sqrt(2048).
All inputs are finite; a program needn't handle non-finite values.
Results may differ from the reference program's by a relative error of at most 0.015.
Values may be sent and summed in bfloat16 or wider, within the bound.
A program may use at most 128 MiB of HBM per device.

```python
import jax
import jax.numpy as jnp
from jax import lax

D = 2048
HEADS = 32
HEAD = 64
GROUP = 2048
BLOCK = 128
SEGMENT = 64
FF = 2816
KCONV = 3
SEQ_LEN = 256
TOKENS = 8192
N_TP = 2


def draw_spatial_proj(key, part):
    key_vals = jax.random.fold_in(key, 11)
    key_cols = jax.random.fold_in(key, 12)
    column = jnp.arange(GROUP).astype(jnp.float32)
    rising = jnp.power(10.0, column / (GROUP - 1))
    jitter = jax.random.uniform(key_cols, (GROUP,), jnp.float32, 0.7, 1.4)
    values = jnp.clip(jax.random.normal(key_vals, (D, GROUP), jnp.float32), -4.0, 4.0)
    return (values * rising * jitter * D ** (-0.5)).astype(jnp.bfloat16)


def level_of(own_key, dims, cuts, smallest, top_value):
    def one(dim, blocks):
        heights = jax.random.uniform(jax.random.fold_in(jax.random.fold_in(own_key, 6), dim), (blocks,), jnp.float32, smallest / len(cuts), top_value / len(cuts))
        return jnp.repeat(jnp.exp(heights), dims[dim] // blocks).reshape((-1,) + (1,) * (len(dims) - dim - 1))

    level = one(*cuts[0])
    for cut in cuts[1:]:
        level = level * one(*cut)
    return level


def bell_draw(own_key, dims, scale, reach, pieces=(), held_as=jnp.bfloat16):
    loudness = level_of(own_key, dims, pieces, -0.22, 0.18) if pieces else 1.0
    drawn = jax.random.normal(own_key, dims, jnp.float32) * scale * loudness
    return jnp.minimum(jnp.maximum(drawn, -reach), reach).astype(held_as)


def setup_inputs(seed: int = 0) -> dict:
    seeds = jax.random.split(jax.random.key(seed), 15)
    residual = bell_draw(seeds[0], (TOKENS, D), 1.0, 6.0, ((0, 32),))
    mixer_gain = jnp.clip(1.0 + 0.18 * jax.random.normal(seeds[1], (D,), jnp.float32), 0.1, 1.9)
    gating_proj = bell_draw(seeds[2], (D, GROUP), D ** -0.5, 0.125, ((0, 8), (1, 2)))
    spatial_proj = draw_spatial_proj(jax.random.fold_in(seeds[14], 71), 0)
    spatial_gain = jnp.clip(1.0 + 0.18 * jax.random.normal(seeds[4], (GROUP,), jnp.float32), 0.1, 1.9)
    spatial_bias = bell_draw(seeds[5], (GROUP,), 0.5, 3.0, (), jnp.float32)
    spatial_mix = bell_draw(seeds[6], (HEADS, BLOCK, BLOCK), BLOCK ** -0.5, 0.5)
    spatial_offset = jnp.clip(jax.random.uniform(seeds[7], (HEADS, BLOCK), jnp.float32, 0.5, 1.5), 0.5, 1.5)
    mixer_out = bell_draw(seeds[8], (GROUP, D), GROUP ** -0.5, 0.125, ((0, 2), (1, 8)))
    channel_gain = jnp.clip(1.0 + 0.18 * jax.random.normal(seeds[9], (D,), jnp.float32), 0.1, 1.9)
    gate_proj = bell_draw(seeds[10], (D, FF), D ** -0.5, 0.125, ((0, 8), (1, 2)))
    up_proj = bell_draw(seeds[11], (D, FF), D ** -0.5, 0.125, ((0, 8), (1, 2)))
    conv_taps = bell_draw(seeds[12], (KCONV, FF), KCONV ** -0.5, 3.5, (), jnp.float32)
    down_proj = bell_draw(seeds[13], (FF, D), FF ** -0.5, 0.109375, ((0, 2), (1, 8)))
    return dict(residual=residual, mixer_gain=mixer_gain, gating_proj=gating_proj, spatial_proj=spatial_proj, spatial_gain=spatial_gain, spatial_bias=spatial_bias, spatial_mix=spatial_mix, spatial_offset=spatial_offset, mixer_out=mixer_out, channel_gain=channel_gain, gate_proj=gate_proj, up_proj=up_proj, conv_taps=conv_taps, down_proj=down_proj)


def round_trip(value):
    return lax.optimization_barrier(value.astype(jnp.bfloat16)).astype(jnp.float32)

def rms_normed(value, gain):
    wide = value.astype(jnp.float32)
    scale = lax.rsqrt(lax.optimization_barrier(jnp.mean(wide * wide, axis=-1, keepdims=True)) + 1e-06)
    return (wide * scale * gain).astype(jnp.bfloat16)

def split_sum(left, right, parts):
    rows, inner = left.shape
    left_parts = left.reshape(rows, parts, inner // parts).astype(jnp.float32)
    right_parts = right.reshape(parts, inner // parts, right.shape[1]).astype(jnp.float32)
    terms = jnp.einsum('snc,ncd->nsd', left_parts, right_parts)
    return lax.optimization_barrier(jnp.sum(terms.astype(jnp.bfloat16).astype(jnp.float32), axis=0))

def one_sequence(args):
    rows, mixer_gain, gating_proj, spatial_proj, spatial_gain, spatial_bias, spatial_mix, spatial_offset, mixer_out, channel_gain, gate_proj, up_proj, conv_taps, down_proj = args
    normed = rms_normed(rows, mixer_gain)
    gating = round_trip(jnp.dot(normed, gating_proj, preferred_element_type=jnp.float32))
    spatial = round_trip(jnp.dot(normed, spatial_proj, preferred_element_type=jnp.float32))
    act_u = jax.nn.gelu(gating)
    act_v = jax.nn.gelu(spatial)
    mean = lax.optimization_barrier(jnp.sum(act_v, axis=-1, keepdims=True)) / GROUP
    var = lax.optimization_barrier(jnp.sum(act_v * act_v, axis=-1, keepdims=True)) / GROUP - mean * mean
    vnorm = ((act_v - mean) * lax.rsqrt(var + 1e-05) * spatial_gain + spatial_bias).astype(jnp.bfloat16)
    place = jnp.arange(BLOCK) // SEGMENT
    allowed = place[None, :] <= place[:, None]
    weights = jnp.where(allowed[None], spatial_mix, jnp.zeros_like(spatial_mix)).astype(jnp.float32)
    blocks = vnorm.reshape(SEQ_LEN // BLOCK, BLOCK, HEADS, HEAD).astype(jnp.float32)
    mixed = jnp.einsum('hij,njhd->nihd', weights, blocks) + spatial_offset.T[None, :, :, None]
    gated = (act_u * mixed.reshape(SEQ_LEN, GROUP)).astype(jnp.bfloat16)
    middle = (rows.astype(jnp.float32) + split_sum(gated, mixer_out, N_TP)).astype(jnp.bfloat16)
    normed2 = rms_normed(middle, channel_gain)
    gate = round_trip(jnp.dot(normed2, gate_proj, preferred_element_type=jnp.float32))
    up = round_trip(jnp.dot(normed2, up_proj, preferred_element_type=jnp.float32))
    padded = jnp.concatenate([jnp.zeros((KCONV - 1, FF), jnp.float32), gate], axis=0)
    conv = jnp.zeros((SEQ_LEN, FF), jnp.float32)
    for tap in range(KCONV):
        conv = conv + conv_taps[tap] * padded[tap:tap + SEQ_LEN]
    hidden = (jax.nn.silu(conv) * up).astype(jnp.bfloat16)
    return (middle.astype(jnp.float32) + split_sum(hidden, down_proj, N_TP)).astype(jnp.bfloat16)

def reference(residual, mixer_gain, gating_proj, spatial_proj, spatial_gain, spatial_bias, spatial_mix, spatial_offset, mixer_out, channel_gain, gate_proj, up_proj, conv_taps, down_proj):
    shaped = residual.reshape(residual.shape[0] // SEQ_LEN, SEQ_LEN, D)

    def apply(rows):
        return one_sequence((rows, mixer_gain, gating_proj, spatial_proj, spatial_gain, spatial_bias, spatial_mix, spatial_offset, mixer_out, channel_gain, gate_proj, up_proj, conv_taps, down_proj))
    result = lax.map(apply, shaped)
    return result.reshape(residual.shape[0], D)
```

```python
import jax
import jax.numpy as jnp
from jax import lax
from jax.sharding import PartitionSpec as P

HEAD = 64
GROUP = 2048
BLOCK = 128
SEGMENT = 64
KCONV = 3
SEQ_LEN = 256


def rms_normed(value, gain):
    wide = value.astype(jnp.float32)
    scale = lax.rsqrt(jnp.mean(wide * wide, axis=-1, keepdims=True) + 1e-06)
    return (wide * scale * gain).astype(jnp.bfloat16)


def rotate(value, axis, size, by):
    return lax.ppermute(value, axis, [(i, (i + by) % size) for i in range(size)])


def grid_of(size):
    inner = max(d for d in range(1, size + 1) if size % d == 0 and d * d <= size)
    return size // inner, inner


def along_outer(value, outer, inner, by):
    pairs = [
        (z * inner + y, ((z + by) % outer) * inner + y) for z in range(outer) for y in range(inner)
    ]
    return lax.ppermute(value, "fs", pairs)


def along_inner(value, outer, inner, by):
    pairs = [
        (z * inner + y, z * inner + (y + by) % inner) for z in range(outer) for y in range(inner)
    ]
    return lax.ppermute(value, "fs", pairs)


def gather_fs(owns, fs, after):
    outer, inner = grid_of(fs)
    if after:
        owns, _ = lax.optimization_barrier((owns, after))
    me = lax.axis_index("fs")
    z, y = me // inner, me % inner
    order = sorted(range(1, outer), key=lambda s: -min(s, outer - s))
    lines = {0: owns}
    for s in order:
        lines[s] = [along_outer(own, outer, inner, s) for own in owns]
    wholes = [jnp.zeros((fs,) + own.shape, own.dtype) for own in owns]
    for s in [0] + order:
        for t in range(inner):
            blocks = lines[s] if t == 0 else [along_inner(b, outer, inner, t) for b in lines[s]]
            slot = ((z - s) % outer) * inner + (y - t) % inner
            wholes = [
                lax.dynamic_update_slice(whole, block[None], (slot,) + (0,) * block.ndim)
                for whole, block in zip(wholes, blocks)
            ]
    return wholes, [b for s in order for b in lines[s]]


def gather_rows(own, reps, tps):
    chips = [own] + [rotate(own, "rep", reps, dr) for dr in range(1, reps)]
    slots = []
    for chip in chips:
        slots += [chip] + [rotate(chip, "tp", tps, dc) for dc in range(1, tps)]
    return jnp.concatenate(slots, axis=0)


def scatter_rows(part, reps, tps):
    part = part.reshape((reps, tps, part.shape[0] // (reps * tps)) + part.shape[1:])
    sums = []
    for dr in range(reps):
        total = part[dr, 0].astype(jnp.float32)
        for dc in range(1, tps):
            total = total + rotate(part[dr, dc], "tp", tps, -dc).astype(jnp.float32)
        sums.append(total)
    total = sums[0]
    for dr in range(1, reps):
        total = total + rotate(sums[dr].astype(jnp.bfloat16), "rep", reps, -dr).astype(jnp.float32)
    return total


def sum_group(value, reps, tps):
    shape = value.shape
    value = value.reshape(shape[0], reps, tps, -1)
    for axis, size, dim in (("tp", tps, 2), ("rep", reps, 1)):
        total = value
        for by in range(1, size):
            total = total + jnp.roll(rotate(value, axis, size, by), by, axis=dim)
        value = total
    return value.reshape(shape)


def body(reps, fs, tps):
    def on_device(
        residual,
        mixer_gain,
        gating_proj,
        spatial_proj,
        spatial_gain,
        spatial_bias,
        spatial_mix,
        spatial_offset,
        mixer_out,
        channel_gain,
        gate_proj,
        up_proj,
        conv_taps,
        down_proj,
    ):
        r, c = lax.axis_index("rep"), lax.axis_index("tp")
        rows = residual.shape[0]
        assert rows % SEQ_LEN == 0
        group_rows = rows * reps * tps

        def share(value, dim):
            size = value.shape[dim] // reps
            return lax.dynamic_slice_in_dim(value, r * size, size, dim)

        width = gating_proj.shape[1] // reps
        units = gate_proj.shape[1] // reps
        depth = gating_proj.shape[0] * fs

        normed = gather_rows(rms_normed(residual, mixer_gain), reps, tps)
        (both_w,), sent = gather_fs(
            [jnp.concatenate([share(gating_proj, 1), share(spatial_proj, 1)], axis=1)], fs, []
        )
        (out_w,), sent = gather_fs([share(mixer_out, 0)], fs, sent)
        (gate_w, up_w), sent = gather_fs([share(gate_proj, 1), share(up_proj, 1)], fs, sent)
        (down_w,), sent = gather_fs([share(down_proj, 0)], fs, sent)

        both = jnp.dot(
            normed, both_w.reshape(depth, 2 * width), preferred_element_type=jnp.float32
        ).astype(jnp.bfloat16)
        act_u = jax.nn.gelu(both[:, :width].astype(jnp.float32))
        act_v = jax.nn.gelu(both[:, width:].astype(jnp.float32))
        stats = jnp.stack([jnp.sum(act_v, axis=-1), jnp.sum(act_v * act_v, axis=-1)])
        total, squares = sum_group(stats, reps, tps)
        mean = (total / GROUP)[:, None]
        var = (squares / GROUP)[:, None] - mean * mean
        first = (c * reps + r) * width
        gain_here = lax.dynamic_slice_in_dim(spatial_gain, first, width)
        bias_here = lax.dynamic_slice_in_dim(spatial_bias, first, width)
        vnorm = ((act_v - mean) * lax.rsqrt(var + 1e-05) * gain_here + bias_here).astype(
            jnp.bfloat16
        )
        heads = width // HEAD
        head = (c * reps + r) * heads
        mix_here = lax.dynamic_slice_in_dim(spatial_mix, head, heads, 0)
        offset_here = lax.dynamic_slice_in_dim(spatial_offset, head, heads, 0)
        place = jnp.arange(BLOCK) // SEGMENT
        allowed = place[None, :] <= place[:, None]
        weights = jnp.where(allowed[None], mix_here, jnp.zeros_like(mix_here))
        blocks = vnorm.reshape(group_rows // BLOCK, BLOCK, heads, HEAD)
        mixed = jnp.einsum("hij,njhd->nihd", weights, blocks, preferred_element_type=jnp.float32)
        mixed = mixed + offset_here.T[None, :, :, None]
        gated = (act_u * mixed.reshape(group_rows, width)).astype(jnp.bfloat16)
        model = mixer_out.shape[1] * fs
        part = jnp.einsum("mk,fkn->mfn", gated, out_w, preferred_element_type=jnp.float32)
        mixer_part = scatter_rows(part.astype(jnp.bfloat16).reshape(group_rows, model), reps, tps)
        middle = (residual.astype(jnp.float32) + mixer_part).astype(jnp.bfloat16)

        normed2 = gather_rows(rms_normed(middle, channel_gain), reps, tps)
        gate = jnp.dot(
            normed2, gate_w.reshape(depth, units), preferred_element_type=jnp.float32
        ).astype(jnp.bfloat16).astype(jnp.float32)
        up = jnp.dot(
            normed2, up_w.reshape(depth, units), preferred_element_type=jnp.float32
        ).astype(jnp.bfloat16).astype(jnp.float32)
        taps_here = lax.dynamic_slice_in_dim(conv_taps, (c * reps + r) * units, units, 1)
        offset = jnp.arange(group_rows) % SEQ_LEN
        conv = taps_here[KCONV - 1] * gate
        for lag in range(1, KCONV):
            shifted = jnp.concatenate([jnp.zeros((lag, units), jnp.float32), gate[:-lag]], axis=0)
            shifted = jnp.where((offset >= lag)[:, None], shifted, 0.0)
            conv = conv + taps_here[KCONV - 1 - lag] * shifted
        hidden = (jax.nn.silu(conv) * up).astype(jnp.bfloat16)
        part = jnp.einsum("mk,fkn->mfn", hidden, down_w, preferred_element_type=jnp.float32)
        channel_part = scatter_rows(part.astype(jnp.bfloat16).reshape(group_rows, model), reps, tps)
        return (middle.astype(jnp.float32) + channel_part).astype(jnp.bfloat16)

    return on_device


def solution(mesh):
    in_specs = (
        P(("rep", "fs", "tp"), None),
        P(),
        P("fs", "tp"),
        P("fs", "tp"),
        P(),
        P(),
        P(),
        P(),
        P("tp", "fs"),
        P(),
        P("fs", "tp"),
        P("fs", "tp"),
        P(),
        P("tp", "fs"),
    )
    out_specs = P(("rep", "fs", "tp"), None)
    return jax.shard_map(
        body(mesh.shape["rep"], mesh.shape["fs"], mesh.shape["tp"]),
        mesh=mesh,
        in_specs=in_specs,
        out_specs=out_specs,
        check_vma=False,
    )
```
